32 devices in a mesh: ep: 4 (over y, x), tp: 8 (over z, core).
Axes of the slice: x: 2, y: 2, z: 4, core: 2. Of those that a mesh axis runs over, the one named last changes fastest.
Arguments:
- tokens: bfloat16 [896, 4096], P('ep', 'tp'), may hold values from -6 to 6
- picks: int32 [4, 4, 56], P('ep'), may hold values from 0 to 223, as said below
- pick_weights: float32 [4, 4, 56], P('ep'), may hold values from 0.1 to 1
- gate_weight: bfloat16 [4, 1280, 4096], P('ep', 'tp'), may hold values from -0.09375 to 0.09375
- up_weight: bfloat16 [4, 1280, 4096], P('ep', 'tp'), may hold values from -0.09375 to 0.09375
- down_weight: bfloat16 [4, 1280, 4096], P('ep', None, 'tp'), may hold values from -0.15625 to 0.15625
- dense_gate: bfloat16 [5120, 4096], P('tp'), may hold values from -0.09375 to 0.09375
- dense_up: bfloat16 [5120, 4096], P('tp'), may hold values from -0.09375 to 0.09375
- dense_down: bfloat16 [5120, 4096], P('tp'), may hold values from -0.078125 to 0.078125
- branch_gate: float32 [4096], P('tp'), may hold values from -6 to 6
Outputs:
- mixed: bfloat16 [896, 4096], P('ep', 'tp')
The draws below stay inside these ranges and needn't reach their ends.
Inputs may be any that keep to these rules, and one draw needn't show every extreme that they name: For each block s and expert e, the 56 entries picks[s, e, :] are distinct rows of that block.
All inputs are finite; a program needn't handle non-finite values.
Results may differ from the reference program's by a relative error of at most 0.014.
Values may be sent and summed in bfloat16 or wider, within the bound.
A program may use at most 64 MiB of HBM per device.

```python
import jax
import jax.numpy as jnp

D = 4096
FF = 1280
DF = 5120
TOK_DEV = 224
SLOTS = 56
EXPERTS = 4
TOKENS = 896
N_EP = 4
N_TP = 8


def draw_picks(key, part):
    key_list = jax.random.split(key, N_EP * EXPERTS)

    def one_block(subkey):
        return jax.random.permutation(subkey, TOK_DEV)[:SLOTS]
    orders = jax.vmap(one_block)(key_list)
    return orders.reshape(N_EP, EXPERTS, SLOTS).astype(jnp.int32)


def levels(rng, dims, cuts, smallest, high):
    loudness, own = 1.0, jax.random.fold_in(rng, 6)
    for axis_at, shards_of in cuts:
        heights = jnp.exp(jax.random.uniform(jax.random.fold_in(own, axis_at), (shards_of,), jnp.float32, smallest / len(cuts), high / len(cuts)))
        loudness = loudness * jnp.repeat(heights, dims[axis_at] // shards_of).reshape([-1 if axis == axis_at else 1 for axis in range(len(dims))])
    return loudness


def scatter_about(own_key, dims, spread, reach, cuts=(), kind=jnp.bfloat16):
    gain = levels(own_key, dims, cuts, -0.22, 0.18) if cuts else 1.0
    drawn = jax.random.normal(own_key, dims, jnp.float32) * spread * gain
    return jnp.minimum(jnp.maximum(drawn, -reach), reach).astype(kind)


def setup_inputs(seed: int = 0) -> dict:
    streams_of = jax.random.split(jax.random.key(seed), 11)
    tokens = scatter_about(streams_of[0], (TOKENS, D), 1.0, 6.0, ((0, 4), (1, 8)))
    picks = draw_picks(jax.random.fold_in(streams_of[10], 71), 0)
    pick_weights = jnp.clip(0.1 + 0.9 * jax.random.uniform(streams_of[2], (N_EP, EXPERTS, SLOTS), jnp.float32) ** levels(streams_of[2], (N_EP, EXPERTS, SLOTS), ((0, 4),), -0.2, 0.2), 0.1, 1.0)
    gate_weight = scatter_about(streams_of[3], (EXPERTS, FF, D), D ** -0.5, 0.09375, ((0, 4), (1, 8)))
    up_weight = scatter_about(streams_of[4], (EXPERTS, FF, D), D ** -0.5, 0.09375, ((0, 4), (1, 8)))
    down_weight = scatter_about(streams_of[5], (EXPERTS, FF, D), FF ** -0.5, 0.15625, ((0, 4), (2, 8)))
    dense_gate = scatter_about(streams_of[6], (DF, D), D ** -0.5, 0.09375, ((0, 8),))
    dense_up = scatter_about(streams_of[7], (DF, D), D ** -0.5, 0.09375, ((0, 8),))
    dense_down = scatter_about(streams_of[8], (DF, D), DF ** -0.5, 0.078125, ((0, 8),))
    branch_gate = scatter_about(streams_of[9], (D,), 1.5, 6.0, ((0, 8),), jnp.float32)
    return dict(tokens=tokens, picks=picks, pick_weights=pick_weights, gate_weight=gate_weight, up_weight=up_weight, down_weight=down_weight, dense_gate=dense_gate, dense_up=dense_up, dense_down=dense_down, branch_gate=branch_gate)


def reference(tokens, picks, pick_weights, gate_weight, up_weight, down_weight, dense_gate, dense_up, dense_down, branch_gate):
    offsets = (jnp.arange(N_EP, dtype=jnp.int32) * TOK_DEV)[:, None]
    mixture = jnp.zeros((TOKENS, D), jnp.float32)
    for expert in range(EXPERTS):
        row_index = (picks[:, expert, :] + offsets).reshape(-1).astype(jnp.int32)
        chosen = tokens[row_index]
        gate_value = jnp.dot(chosen, gate_weight[expert].T, preferred_element_type=jnp.float32)
        up_value = jnp.dot(chosen, up_weight[expert].T, preferred_element_type=jnp.float32)
        hidden = (jax.nn.silu(gate_value) * up_value).astype(jnp.bfloat16)
        result = jnp.dot(hidden, down_weight[expert], preferred_element_type=jnp.float32).astype(jnp.bfloat16)
        weights = pick_weights[:, expert, :].reshape(-1, 1)
        mixture = mixture.at[row_index].add(result.astype(jnp.float32) * weights)
    dense_gval = jnp.dot(tokens, dense_gate.T, preferred_element_type=jnp.float32)
    dense_uval = jnp.dot(tokens, dense_up.T, preferred_element_type=jnp.float32)
    dense_hidden = (jax.nn.silu(dense_gval) * dense_uval).astype(jnp.bfloat16)
    block_width = DF // N_TP
    dense_out = jnp.zeros((TOKENS, D), jnp.float32)
    for block_index in range(N_TP):
        lower = block_index * block_width
        partial_value = jnp.dot(dense_hidden[:, lower:lower + block_width], dense_down[lower:lower + block_width], preferred_element_type=jnp.float32)
        dense_out = dense_out + partial_value.astype(jnp.bfloat16).astype(jnp.float32)
    mixed = mixture + jax.nn.sigmoid(branch_gate)[None, :] * dense_out
    return mixed.astype(jnp.bfloat16)
```

```python
import functools

import jax
import jax.numpy as jnp
from jax import lax
from jax.experimental import pallas as pl
from jax.experimental.pallas import tpu as pltpu
from jax.sharding import PartitionSpec as P

MESH = pl.DeviceIdType.MESH
BF = jnp.bfloat16
F32 = jnp.float32
CORES = 2
R = 2
NT = (((1,), (1,)), ((), ()))
NN = (((1,), (0,)), ((), ()))
TN = (((0,), (0,)), ((), ()))
scope = jax.named_scope


def mm(a, b, dims=NN):
    return lax.dot_general(a, b, dims, preferred_element_type=F32)


def silu(v):
    return v / (1.0 + jnp.exp(-v))


def kernel(
    n_ep, n_tp, pad, F,
    tok_hbm, pk_in, pw_in, weg_hbm, weu_hbm, wed_hbm, wg_hbm, wu_hbm, wd_hbm, bg,
    out_ref,
    x, w, wd, we, wed, acc, oh, whi, wlo, pk, ch, acc_e,
    hx, acc_o, eo, back, hd, ps, pr, own, ru, rd, su, sd, acc_d,
    w_sem, ag_recv, ag_up, ag_dn, ag_pt, c_recv, c_send, cf_recv, cf_send,
    h_recv, h_send, hf_recv, hf_send, e_recv, e_send, p_recv, p_send,
    ru_recv, ru_send, rd_recv, rd_send,
):
    nz = n_tp // CORES
    rows, df = x.shape[1], x.shape[2]
    dl = F * df
    rc = rows // R
    hdn = hd.shape[1]
    he = hx.shape[1]
    s = lax.axis_index("ep")
    t = lax.axis_index("tp")
    z = t // CORES
    c = t % CORES
    partner = CORES * z + (1 - c)
    low = 2 * z < nz - 1
    end = (z == 0) | (z == nz - 1)
    mid = (z > 0) & (z < nz - 1)

    def load(i, src, dst):
        return pltpu.make_async_copy(src, dst, w_sem.at[i])

    tok_loads = [
        load(6 + f, tok_hbm.at[:, pl.ds(f * df, df)], x.at[t * F + f]) for f in range(F)
    ]
    loads = [
        load(0, wg_hbm, w.at[pl.ds(0, hdn), :]),
        load(1, wu_hbm, w.at[pl.ds(hdn, hdn), :]),
        load(2, wd_hbm, wd),
        load(3, weg_hbm, we.at[pl.ds(0, he), :]),
        load(4, weu_hbm, we.at[pl.ds(he, he), :]),
        load(5, wed_hbm, wed),
    ]
    barrier = pltpu.get_barrier_semaphore()
    for cp in tok_loads:
        cp.start()
    pl.semaphore_signal(barrier, inc=1, device_id={"tp": partner}, device_id_type=MESH)

    @pl.when(z > 0)
    def _():
        pl.semaphore_signal(
            barrier, inc=1, device_id={"tp": jnp.maximum(t - CORES, c)}, device_id_type=MESH
        )

    @pl.when(z < nz - 1)
    def _():
        pl.semaphore_signal(
            barrier, inc=1, device_id={"tp": jnp.minimum(t + CORES, n_tp - CORES + c)},
            device_id_type=MESH,
        )

    for k in range(1, n_ep):
        pl.semaphore_signal(barrier, inc=1, device_id={"ep": (s + k) % n_ep}, device_id_type=MESH)
    for cp in loads:
        cp.start()

    def remote(src, dst, ssem, rsem, **dev):
        return pltpu.make_async_remote_copy(
            src_ref=src, dst_ref=dst, send_sem=ssem, recv_sem=rsem,
            device_id=dev, device_id_type=MESH,
        )

    def rws(r):
        return pl.ds(r * rc, rc)

    up_dev = jnp.minimum(t + CORES, n_tp - CORES + c)
    dn_dev = jnp.maximum(t - CORES, c)

    def ag_copy(zi, f, r, ssem, dev):
        b = (CORES * zi + c) * F + f
        ref = x.at[b, rws(r), :]
        return remote(ref, ref, ssem.at[zi * F + f, r], ag_recv.at[b, r], tp=dev)

    def ag_wait(j, f, r):
        b = j * F + f
        ref = x.at[b, rws(r), :]
        remote(ref, ref, ag_pt.at[0, 0], ag_recv.at[b, r], tp=partner).wait_recv()

    def c_copy(b, blk, e, src_rows, dst_rows, sem_e, rsem_e):
        return remote(
            pk.at[b, pl.ds(pl.multiple_of(src_rows, pad), pad), :],
            ch.at[blk, pl.ds(pl.multiple_of(dst_rows, pad), pad), :],
            c_send.at[b, sem_e], c_recv.at[b, rsem_e], ep=e,
        )

    def cf_copy(zi, f, core):
        ref = ch.at[(CORES * zi + core) * F + f]
        return remote(ref, ref, cf_send.at[zi * F + f], cf_recv.at[zi * F + f], tp=partner)

    def cols(b):
        return pl.ds(pl.multiple_of(b * df, df), df)

    def wide(j):
        return pl.ds(pl.multiple_of(j * dl, dl), dl)

    near = jnp.minimum(z, nz - 1 - z)

    def order(m):
        both = z + (1 - 2 * (m % 2)) * ((m + 1) // 2)
        far = jnp.where(2 * z < nz - 1, z + m - near, z - m + near)
        return jnp.where(m <= 2 * near, both, far)

    def send_on(zi, f, r):
        @pl.when((zi <= z) & (z < nz - 1))
        def _():
            ag_copy(zi, f, r, ag_up, up_dev).start()

        @pl.when((zi >= z) & (z > 0))
        def _():
            ag_copy(zi, f, r, ag_dn, dn_dev).start()

        ag_copy(zi, f, r, ag_pt, partner).start()

    def forward(zi, r):
        for f in range(F):
            ag_wait(CORES * zi + c, f, r)
            send_on(zi, f, r)

    with scope("tokwait"):
        for cp in tok_loads:
            cp.wait()
    with scope("barrier"):
        pl.semaphore_wait(
            barrier,
            n_ep + jnp.where(z > 0, 1, 0) + jnp.where(z < nz - 1, 1, 0),
        )
    for r in range(R):
        for f in range(F):
            send_on(z, f, r)

    slots = pk_in.shape[2]
    ep_rows = n_ep * pad
    spread = (
        lax.broadcasted_iota(jnp.int32, (pad, slots), 0)
        == lax.broadcasted_iota(jnp.int32, (pad, slots), 1)
    ).astype(F32).astype(BF)

    with scope("prep"):
        for e in range(n_ep):
            ids = lax.broadcasted_iota(jnp.int32, (rows, slots), 0)
            hit = ids == pk_in[0, pl.ds(e, 1), :]
            oh[e * pad:(e + 1) * pad, :] = mm(spread, hit.astype(F32).astype(BF), NT).astype(BF)
        place_hi = jnp.zeros((rows, ep_rows), F32)
        place_lo = jnp.zeros((rows, ep_rows), F32)
        for e in range(n_ep):
            ids = lax.broadcasted_iota(jnp.int32, (rows, slots), 0)
            sel = jnp.where(ids == pk_in[0, pl.ds(e, 1), :], pw_in[0, pl.ds(e, 1), :], 0.0)
            hi = sel.astype(BF)
            lo = (sel - hi.astype(F32)).astype(BF)
            at = (
                lax.broadcasted_iota(jnp.int32, (slots, ep_rows), 0) + e * pad
                == lax.broadcasted_iota(jnp.int32, (slots, ep_rows), 1)
            ).astype(F32).astype(BF)
            place_hi += mm(hi, at)
            place_lo += mm(lo, at)
        whi[...] = place_hi.astype(BF)
        wlo[...] = place_lo.astype(BF)
        acc[...] = jnp.zeros_like(acc)
        acc_e[...] = jnp.zeros_like(acc_e)
        acc_o[...] = jnp.zeros_like(acc_o)

    def dense_block(j, r):
        v = mm(x[j * F, rws(r), :], w[:, cols(j * F)], NT)
        for f in range(1, F):
            v += mm(x[j * F + f, rws(r), :], w[:, cols(j * F + f)], NT)
        acc[rws(r), :] += v

    def pick(zi):
        mine = (CORES * zi + c) * F
        for f in range(F):
            b = zi * F + f
            pk[b] = mm(oh[...], x[mine + f]).astype(BF)
            for k in range(1, n_ep):
                e = (s + n_ep - k) % n_ep
                c_copy(b, mine + f, e, e * pad, s * pad, e, s).start()
            keep = pl.ds(pl.multiple_of(s * pad, pad), pad)
            ch[mine + f, keep, :] = pk[b, keep, :]

    def dense_pair(zi, r):
        with scope("dmine"):
            dense_block(CORES * zi + c, r)
        other = CORES * zi + (1 - c)
        with scope("dwait"):
            for f in range(F):
                ag_wait(other, f, r)
        with scope("dother"):
            dense_block(other, r)

    def p_copy(zi, r):
        return remote(
            ps.at[zi, rws(r), :], pr.at[zi, rws(r), :],
            p_send.at[zi, r], p_recv.at[zi, r], tp=partner,
        )

    def rs_up(zu, f, r, src):
        b = zu * F + f
        return remote(src.at[b, rws(r), :], ru.at[b, rws(r), :],
                      ru_send.at[b, r], ru_recv.at[b, r], tp=up_dev)

    def rs_dn(zd, f, r, src):
        b = zd * F + f
        return remote(src.at[b, rws(r), :], rd.at[b, rws(r), :],
                      rd_send.at[b, r], rd_recv.at[b, r], tp=dn_dev)

    def partials(r):
        def far(i):
            return jnp.where(low, nz - 1 - i, i)

        with scope("ps"):
            @pl.loop(0, nz)
            def _(i):
                zi = far(i)
                ps[zi, rws(r), :] = mm(
                    hd[rws(r), :], wd[:, wide(CORES * zi + (1 - c))]
                ).astype(BF)
                p_copy(zi, r).start()

        with scope("own"):
            @pl.loop(0, nz)
            def _(i):
                zi = far(i)
                v = mm(hd[rws(r), :], wd[:, wide(CORES * zi + c)])
                p_copy(zi, r).wait_recv()
                v += pr[zi, rws(r), :].astype(F32)
                for f in range(F):
                    own[zi * F + f, rws(r), :] = v[:, f * df:(f + 1) * df].astype(BF)

                @pl.when((z == 0) & (zi > z))
                def _():
                    for f in range(F):
                        rs_up(zi, f, r, own).start()

                @pl.when((z == nz - 1) & (zi < z))
                def _():
                    for f in range(F):
                        rs_dn(zi, f, r, own).start()

    for r in range(R):
        last = r == R - 1

        @pl.loop(0, nz)
        def _(m):
            zi = order(m)

            @pl.when((m > 0) & ((jnp.abs(zi - z) > 1) | (r == 0)))
            def _():
                with scope(f"fwd{r}"):
                    forward(zi, r)

            if last:
                with scope("pick"):
                    pick(zi)
            if r == 0:
                @pl.when(m == 0)
                def _():
                    with scope("wload"):
                        loads[0].wait()
                        loads[1].wait()
            dense_pair(zi, r)

        if not last:
            with scope("fwdnear"):
                @pl.when(z > 0)
                def _():
                    forward(jnp.maximum(z - 1, 0), r + 1)

                @pl.when(z < nz - 1)
                def _():
                    forward(jnp.minimum(z + 1, nz - 1), r + 1)

        hid = acc[rws(r), :]
        hd[rws(r), :] = (silu(hid[:, :hdn]) * hid[:, hdn:]).astype(BF)
        if r == 0:
            loads[2].wait()
        if not last:
            @pl.when(end)
            def _():
                partials(r)
        else:
            @pl.when(mid)
            def _():
                for q in range(R - 1):
                    partials(q)

            partials(r)

    loads[3].wait()
    loads[4].wait()

    def emm(j):
        with scope("emm"):
            v = mm(we[:, cols(j * F)], ch[j * F], NT)
            for f in range(1, F):
                v += mm(we[:, cols(j * F + f)], ch[j * F + f], NT)
            acc_e[...] += v

    def emm_other(zi):
        with scope("cfwait"):
            for f in range(F):
                cf_copy(zi, f, 1 - c).wait_recv()
        emm(CORES * zi + (1 - c))

    @pl.loop(0, nz)
    def _(m):
        zi = order(m)
        mine = (CORES * zi + c) * F
        with scope("cwait"):
            for f in range(F):
                for k in range(1, n_ep):
                    e = (s + k) % n_ep
                    c_copy(zi * F + f, mine + f, e, e * pad, e * pad, e, e).wait_recv()
                cf_copy(zi, f, c).start()
        emm(CORES * zi + c)

        @pl.when(m > 0)
        def _():
            emm_other(order(jnp.maximum(m - 1, 0)))

    emm_other(order(nz - 1))
    he_acc = acc_e[...]
    hx[t] = (silu(he_acc[:he]) * he_acc[he:]).astype(BF)

    def h_copy(zo, src_z, sidx):
        ref = hx.at[CORES * src_z + c]
        return remote(ref, ref, h_send.at[sidx], h_recv.at[src_z], tp=CORES * zo + c)

    def hf_copy(zi, core):
        ref = hx.at[CORES * zi + core]
        return remote(ref, ref, hf_send.at[zi], hf_recv.at[zi], tp=partner)

    for k in range(1, nz):
        zo = (z + k) % nz
        h_copy(zo, z, zo).start()
    hf_copy(z, c).start()

    def turn(zu, f, r, hop, got, out, cond, name):
        @pl.when(cond)
        def _():
            with scope(name):
                b = zu * F + f
                hop(zu, f, r, out).wait_recv()
                out[b, rws(r), :] = (
                    own[b, rws(r), :].astype(F32) + got[b, rws(r), :].astype(F32)
                ).astype(BF)
                hop(zu, f, r, out).start()

    def ups(r, lo_i, hi_i):
        @pl.loop(lo_i, hi_i)
        def _(i):
            zu = nz - 1 - i
            for f in range(F):
                turn(zu, f, r, rs_up, ru, su, zu > z, f"up{r}")

    def dns(r, lo_i, hi_i):
        @pl.loop(lo_i, hi_i)
        def _(i):
            for f in range(F):
                turn(i, f, r, rs_dn, rd, sd, i < z, f"dn{r}")

    def relay(r, lo_i, hi_i, second):
        @pl.when(mid & low)
        def _():
            ups(r, lo_i, hi_i)
            if second:
                dns(r, 0, nz - 1)

        @pl.when(mid & jnp.logical_not(low))
        def _():
            dns(r, lo_i, hi_i)
            if second:
                ups(r, 0, nz - 1)

    for r in range(R - 1):
        relay(r, 0, nz - 1, True)
    relay(R - 1, 0, 1, False)

    loads[5].wait()

    def down(j):
        acc_o[...] += mm(hx[j], wed[j], TN)

    def down_other(zi):
        with scope("hfwait"):
            hf_copy(zi, 1 - c).wait_recv()
        with scope("down"):
            down(CORES * zi + (1 - c))

    @pl.loop(0, nz)
    def _(m):
        zi = order(m)

        @pl.when(zi != z)
        def _():
            with scope("hwait"):
                h_copy((z + 1) % nz, zi, z).wait_recv()
                hf_copy(zi, c).start()

        with scope("down"):
            down(CORES * zi + c)

        @pl.when(m > 0)
        def _():
            down_other(order(jnp.maximum(m - 1, 0)))

    down_other(order(nz - 1))
    eo[...] = acc_o[...].astype(BF)

    def e_copy(dev, src_i, dst_i, ssem, rsem):
        return remote(
            eo.at[pl.ds(pl.multiple_of(src_i * pad, pad), pad), :],
            back.at[pl.ds(pl.multiple_of(dst_i * pad, pad), pad), :],
            e_send.at[ssem], e_recv.at[rsem], ep=dev,
        )

    for k in range(1, n_ep):
        e = (s + n_ep - k) % n_ep
        e_copy(e, e, s, e, s).start()
    keep = pl.ds(pl.multiple_of(s * pad, pad), pad)
    back[keep, :] = eo[keep, :]

    relay(R - 1, 1, nz - 1, True)

    for f in range(F):
        acc_d[:, f * df:(f + 1) * df] = own[z * F + f].astype(F32)

    def finish(hop, got):
        for r in range(R):
            for f in range(F):
                hop(z, f, r, su).wait_recv()
                acc_d[rws(r), f * df:(f + 1) * df] += got[z * F + f, rws(r), :].astype(F32)

    @pl.when(z > 0)
    def _():
        with scope("finup"):
            finish(rs_up, ru)

    @pl.when(z < nz - 1)
    def _():
        with scope("findn"):
            finish(rs_dn, rd)

    acc_d[...] = acc_d[...] * (1.0 / (1.0 + jnp.exp(-bg[...])))

    with scope("sends"):
        @pl.loop(0, nz)
        def _(zi):
            for f in range(F):
                b = zi * F + f
                for r in range(R):
                    @pl.when((zi <= z) & (z < nz - 1))
                    def _():
                        ag_copy(zi, f, r, ag_up, up_dev).wait_send()

                    @pl.when((zi >= z) & (z > 0))
                    def _():
                        ag_copy(zi, f, r, ag_dn, dn_dev).wait_send()

                    ag_copy(zi, f, r, ag_pt, partner).wait_send()

                    @pl.when((zi > z) & (z < nz - 1))
                    def _():
                        rs_up(zi, f, r, su).wait_send()

                    @pl.when((zi < z) & (z > 0))
                    def _():
                        rs_dn(zi, f, r, sd).wait_send()

                for k in range(1, n_ep):
                    e = (s + k) % n_ep
                    c_copy(b, (CORES * zi + c) * F + f, e, e * pad, s * pad, e, s).wait_send()
                cf_copy(zi, f, c).wait_send()
            for r in range(R):
                p_copy(zi, r).wait_send()
            hf_copy(zi, c).wait_send()

            @pl.when(zi != z)
            def _():
                h_copy((z + 1) % nz, z, zi).wait_send()

    with scope("ewait"):
        for k in range(1, n_ep):
            e = (s + k) % n_ep
            e_copy(e, e, e, e, e).wait_recv()
    with scope("combine"):
        out_ref[...] = (
            acc_d[...] + (mm(whi[...], back[...]) + mm(wlo[...], back[...]))
        ).astype(BF)

    for k in range(1, n_ep):
        e = (s + k) % n_ep
        e_copy(e, e, s, e, s).wait_send()


def per_device(
    n_ep, n_tp, tokens, picks, pick_weights, gate_weight, up_weight, down_weight,
    dense_gate, dense_up, dense_down, branch_gate,
):
    rows, dl = tokens.shape
    slots = picks.shape[2]
    pad = -(-slots // 16) * 16
    nz = n_tp // CORES
    he, width = gate_weight.shape[1], gate_weight.shape[2]
    hd = dense_gate.shape[0]
    ep_rows = n_ep * pad
    F = 2 if dl % 256 == 0 else 1
    df = dl // F
    vm = pl.BlockSpec(memory_space=pltpu.VMEM)
    hbm = pl.BlockSpec(memory_space=pl.ANY)
    sem = pltpu.SemaphoreType.DMA
    parts = pltpu.VMEM((nz * F, rows, df), BF)
    return pl.pallas_call(
        functools.partial(kernel, n_ep, n_tp, pad, F),
        out_shape=jax.ShapeDtypeStruct((rows, dl), BF),
        in_specs=[hbm, vm, vm, hbm, hbm, hbm, hbm, hbm, hbm, vm],
        out_specs=vm,
        scratch_shapes=[
            pltpu.VMEM((n_tp * F, rows, df), BF),
            pltpu.VMEM((2 * hd, width), BF),
            pltpu.VMEM((hd, width), BF),
            pltpu.VMEM((2 * he, width), BF),
            pltpu.VMEM((n_tp, he, dl), BF),
            pltpu.VMEM((rows, 2 * hd), F32),
            pltpu.VMEM((ep_rows, rows), BF),
            pltpu.VMEM((rows, ep_rows), BF),
            pltpu.VMEM((rows, ep_rows), BF),
            pltpu.VMEM((nz * F, ep_rows, df), BF),
            pltpu.VMEM((n_tp * F, ep_rows, df), BF),
            pltpu.VMEM((2 * he, ep_rows), F32),
            pltpu.VMEM((n_tp, he, ep_rows), BF),
            pltpu.VMEM((ep_rows, dl), F32),
            pltpu.VMEM((ep_rows, dl), BF),
            pltpu.VMEM((ep_rows, dl), BF),
            pltpu.VMEM((rows, hd), BF),
            pltpu.VMEM((nz, rows, dl), BF),
            pltpu.VMEM((nz, rows, dl), BF),
            parts, parts, parts, parts, parts,
            pltpu.VMEM((rows, dl), F32),
            sem((6 + F,)),
            sem((n_tp * F, R)), sem((nz * F, R)), sem((nz * F, R)), sem((nz * F, R)),
            sem((nz * F, n_ep)), sem((nz * F, n_ep)), sem((nz * F,)), sem((nz * F,)),
            sem((nz,)), sem((nz,)), sem((nz,)), sem((nz,)),
            sem((n_ep,)), sem((n_ep,)), sem((nz, R)), sem((nz, R)),
            sem((nz * F, R)), sem((nz * F, R)), sem((nz * F, R)), sem((nz * F, R)),
        ],
        compiler_params=pltpu.CompilerParams(
            collective_id=0, has_side_effects=True, vmem_limit_bytes=60 * 1024 * 1024
        ),
    )(
        tokens, picks, pick_weights,
        gate_weight[0], up_weight[0], down_weight[0].reshape(n_tp, he, dl),
        dense_gate, dense_up, dense_down, branch_gate.reshape(1, -1),
    )


def solution(mesh):
    in_specs = (
        P("ep", "tp"),
        P("ep", None, None),
        P("ep", None, None),
        P("ep", "tp", None),
        P("ep", "tp", None),
        P("ep", None, "tp"),
        P("tp", None),
        P("tp", None),
        P("tp", None),
        P("tp"),
    )
    return jax.shard_map(
        functools.partial(per_device, mesh.shape["ep"], mesh.shape["tp"]),
        mesh=mesh, in_specs=in_specs, out_specs=P("ep", "tp"), check_vma=False,
    )
```
